32 devices in a mesh: sp: 4 (over y, x), tp: 8 (over z, core).
Axes of the slice: x: 2, y: 2, z: 4, core: 2. Of those that a mesh axis runs over, the one named last changes fastest.
Arguments:
- queries: bfloat16 [2048, 2048], P('sp', 'tp'), may hold values from -8 to 8
- keys: bfloat16 [2048, 1024], P('sp', 'tp'), may hold values from -8 to 8
- values: bfloat16 [2048, 1024], P('sp', 'tp'), may hold values from -6 to 6
- doc_ids: int32 [2048], P('sp'), may hold values from 0 to 1, never falling along the last dimension, each value on 1 to 1536 neighbouring positions
- sink_logits: float32 [32], P('tp'), may hold values from 3 to 6
- out_weight: bfloat16 [2048, 2048], P('tp'), may hold values from -0.75 to 0.75
- residual: bfloat16 [2048, 2048], P(('sp', 'tp')), may hold values from -6 to 6
- norm_gain: float32 [2048], replicated, may hold values from 0.1 to 1.9
- routes: int32 [2048, 2], P(('sp', 'tp')), may hold values from 0 to 3, all different within a row; in each aligned block of 64 rows (0 to 63, 64 to 127, ...) at most 36 rows name the same one
- route_weights: float32 [2048, 2], P(('sp', 'tp')), may hold values from 0.2 to 1
- gate_weight: bfloat16 [4, 2048, 7168], P('sp', None, 'tp'), may hold values from -0.125 to 0.125
- up_weight: bfloat16 [4, 2048, 7168], P('sp', None, 'tp'), may hold values from -0.125 to 0.125
- down_weight: bfloat16 [4, 7168, 2048], P('sp', 'tp'), may hold values from -0.0625 to 0.0625
Outputs:
- layer_output: bfloat16 [2048, 2048], P(('sp', 'tp'))
The draws below stay inside these ranges and needn't reach their ends.
Inputs may be any that keep to these rules, and one draw needn't show every extreme that they name: `doc_ids`: never falling along the sequence; each document spans 1 to 1536 positions, one exactly that many. `routes`: each row names 2 different experts. In the rows of one device (aligned blocks of 64 rows) no expert is named by more than 36 rows, a bound that some block reaches.
All inputs are finite; a program needn't handle non-finite values.
Results may differ from the reference program's by a relative error of at most 0.015.
Values may be sent and summed in bfloat16 or wider, within the bound.
No kernel may reach another device: no remote copies, remote signals or barrier semaphores. Data moves between devices by JAX's collectives and lax.ppermute only.
A program may use at most 128 MiB of HBM per device.

```python
import math
import jax
import jax.numpy as jnp
import numpy as np
from jax import lax

D = 2048
HEADS = 32
KV_HEADS = 16
HEAD_DIM = 64
WINDOW = 128
FF = 7168
TOP_K = 2
TOK_DEV = 64
TOK_SP = 512
SEQ = 2048
EXPERTS = 4
CAP = 36
DOCS = 2
N_TP = 8


def draw_queries(key, part):
    normal_values = jnp.clip(jax.random.normal(jax.random.fold_in(key, 1), (SEQ, HEADS * HEAD_DIM), jnp.float32), -6.0, 6.0)
    return normal_values.astype(jnp.bfloat16)


def draw_keys(key, part):
    normal_values = jnp.clip(jax.random.normal(jax.random.fold_in(key, 2), (SEQ, KV_HEADS * HEAD_DIM), jnp.float32), -6.0, 6.0)
    return normal_values.astype(jnp.bfloat16)


def block_scale(rng, dims, cuts, smallest, top_value):
    level = 1.0
    for axis_at, parts in cuts:
        heights = jax.random.uniform(jax.random.fold_in(jax.random.fold_in(rng, 6), axis_at), (parts,), jnp.float32, smallest / len(cuts), top_value / len(cuts))
        level = level * jnp.repeat(jnp.exp(heights), dims[axis_at] // parts).reshape((-1,) + (1,) * (len(dims) - 1 - axis_at))
    return level


def length_profile(amount, total, limit, skew):
    portions = [(1 << 20) // math.isqrt(grade ** skew) + 1 for grade in range(2, amount + 1)]
    surplus, given = total - limit - (amount - 1), [1] * (amount - 1)
    while surplus > 0:
        movable = [i for i in range(amount - 1) if given[i] < limit]
        mass, remaining = sum([portions[i] for i in movable]), surplus
        for i in movable:
            more = min(limit - given[i], max(1, remaining * portions[i] // mass), surplus)
            given[i] = given[i] + more
            surplus = surplus - more
    return np.array([limit] + given)


def ragged_sizes(stream_key, number_of, total, most, skew):
    if number_of == 2:
        one = jax.random.randint(stream_key, (), max(1, total - most), min(most, total - 1) + 1)
        return jnp.stack([one, total - one])
    lengths = jnp.asarray(length_profile(number_of, total, most, skew), jnp.int32)
    twos = (number_of - 1) // 2
    donor, sink = lengths[1:1 + 2 * twos:2], lengths[2:2 + 2 * twos:2]
    slack = jnp.minimum(donor - 1, most - sink)
    passed = jax.random.randint(jax.random.fold_in(stream_key, 1), (twos,), 0, 1 << 20) % (slack + 1)
    lengths = lengths.at[1:1 + 2 * twos:2].set(donor - passed).at[2:2 + 2 * twos:2].set(sink + passed)
    return lengths[jax.random.permutation(jax.random.fold_in(stream_key, 2), number_of)]


def deal_out(own_key, own, number, rows, number_of, top, reach, lean):
    order = jax.random.permutation(own_key, number_of)
    heavy_load, ordinary = load_shares(number_of, rows * top, reach, lean, True), load_shares(number_of, rows * top, reach, lean, False)
    places = jnp.arange(number_of)

    def named(sizes, turn):
        used = int((sizes > 0).sum())
        fixed = max(1, used // 4)
        passed = fixed + (places - fixed + turn * (used - fixed)) % max(1, number_of - fixed)
        return jnp.zeros((number_of,), jnp.int32).at[order[jnp.where(places < fixed, places, passed)]].set(jnp.asarray(sizes, jnp.int32))

    sizes = jnp.where(number % 4 == 0, named(heavy_load, number // 4), named(ordinary, number - number // 4 - 1))
    mixed = jax.random.permutation(jax.random.fold_in(own, 3), number_of)
    donor, sink = mixed[0:number_of // 2 * 2:2], mixed[1:number_of // 2 * 2:2]
    margin = jnp.minimum(sizes[donor] - 1, reach - sizes[sink]) // 2
    margin = jnp.where((donor == order[0]) | (sink == order[0]) | (sizes[sink] == 0), 0, jnp.maximum(margin, 0))
    passed = jax.random.randint(jax.random.fold_in(own, 4), (number_of // 2,), 0, 1 << 20) % (margin + 1)
    sizes = sizes.at[donor].add(-passed).at[sink].add(passed)
    labels = jnp.searchsorted(jnp.cumsum(sizes), jnp.arange(rows * top), side="right").astype(jnp.int32)
    listing = labels.reshape(top, rows).T
    listing = listing[jax.random.permutation(jax.random.fold_in(own, 1), rows)]
    turn = jax.random.randint(jax.random.fold_in(own, 2), (rows, 1), 0, top)
    return jnp.take_along_axis(listing, (jnp.arange(top)[None, :] + turn) % top, axis=1)


def load_shares(number_of, total, limit, skew, full):
    loads = [(1 << 20) // math.isqrt(rank ** skew) + 1 for rank in range(1, number_of + 1)]
    largest = limit if full else min(limit, max(-(-total // number_of), total * loads[0] // sum(loads)))
    least = 1 if total - largest >= number_of - 1 else 0
    counts, surplus = [largest] + [least] * (number_of - 1), total - largest - least * (number_of - 1)
    while surplus > 0:
        free = [i for i in range(1, number_of) if counts[i] < largest] or [i for i in range(1, number_of) if counts[i] < limit]
        mass, left = sum([loads[i] for i in free]), surplus
        for i in free:
            extra = min(limit - counts[i], max(1, left * loads[i] // mass), surplus)
            counts[i] = counts[i] + extra
            surplus = surplus - extra
    return np.array(counts)


def noise(own_key, extent, scale, reach, cuts=(), kind=jnp.bfloat16):
    entries = scale * jax.random.normal(own_key, extent, jnp.float32)
    if cuts:
        entries = entries * block_scale(own_key, extent, cuts, -0.22, 0.18)
    return jnp.clip(entries, -reach, reach).astype(kind)


def setup_inputs(seed: int = 0) -> dict:
    key_of = jax.random.split(jax.random.key(seed), 14)
    queries = draw_queries(jax.random.fold_in(key_of[13], 71), 0)
    keys = draw_keys(jax.random.fold_in(key_of[13], 71), 0)
    values = noise(key_of[2], (SEQ, KV_HEADS * HEAD_DIM), 1.0, 6.0, ((0, 4), (1, 8)))
    doc_ids = jnp.searchsorted(jnp.cumsum(ragged_sizes(key_of[3], DOCS, SEQ, 3 * TOK_SP, 1)), jnp.arange(SEQ), side="right").astype(jnp.int32)
    sink_logits = jnp.clip(3.0 + 3.0 * jax.random.uniform(key_of[4], (HEADS,), jnp.float32) ** block_scale(key_of[4], (HEADS,), ((0, 8),), -0.2, 0.2), 3.0, 6.0)
    out_weight = noise(key_of[5], (HEADS * HEAD_DIM, D), HEAD_DIM ** -0.5, 0.75, ((0, 8),))
    residual = noise(key_of[6], (SEQ, D), 1.0, 6.0, ((0, 32),))
    norm_gain = jnp.clip(1.0 + 0.18 * jax.random.normal(key_of[7], (D,), jnp.float32), 0.1, 1.9)
    routes_keys = jax.random.split(jax.random.fold_in(key_of[8], 1), SEQ // TOK_DEV)
    routes_turns = jax.random.permutation(jax.random.fold_in(key_of[8], 3), SEQ // TOK_DEV)
    routes = jax.vmap(lambda own, number: deal_out(jax.random.fold_in(key_of[8], 2), own, number, TOK_DEV, EXPERTS, TOP_K, CAP, 2))(routes_keys, routes_turns).reshape((SEQ, TOP_K))
    route_weights = jnp.clip(0.2 + 0.8 * jax.random.uniform(key_of[9], (SEQ, TOP_K), jnp.float32) ** block_scale(key_of[9], (SEQ, TOP_K), ((0, 32),), -0.2, 0.2), 0.2, 1.0)
    gate_weight = noise(key_of[10], (EXPERTS, D, FF), D ** -0.5, 0.125, ((0, 4), (2, 8)))
    up_weight = noise(key_of[11], (EXPERTS, D, FF), D ** -0.5, 0.125, ((0, 4), (2, 8)))
    down_weight = noise(key_of[12], (EXPERTS, FF, D), FF ** -0.5, 0.0625, ((0, 4), (1, 8)))
    return dict(queries=queries, keys=keys, values=values, doc_ids=doc_ids, sink_logits=sink_logits, out_weight=out_weight, residual=residual, norm_gain=norm_gain, routes=routes, route_weights=route_weights, gate_weight=gate_weight, up_weight=up_weight, down_weight=down_weight)


layer_epsilon = 1e-05
masked_score = -1e+30

def reference(queries, keys, values, doc_ids, sink_logits, out_weight, residual, norm_gain, routes, route_weights, gate_weight, up_weight, down_weight):
    reach_back = WINDOW - 1
    group_ratio = HEADS // KV_HEADS
    block_rows = min(512, TOK_SP)
    score_scale = 1.0 / math.sqrt(HEAD_DIM)
    kv_width = KV_HEADS * HEAD_DIM
    padded_keys = jnp.concatenate([jnp.zeros((reach_back, kv_width), keys.dtype), keys], axis=0)
    padded_values = jnp.concatenate([jnp.zeros((reach_back, kv_width), values.dtype), values], axis=0)
    padded_docs = jnp.concatenate([jnp.full((reach_back,), -1, jnp.int32), doc_ids.astype(jnp.int32)], axis=0)
    sink_table = sink_logits.astype(jnp.float32).reshape(KV_HEADS, group_ratio, 1)

    def attend_block(block_index):
        first_row = (block_index * block_rows).astype(jnp.int32)
        query_rows = lax.dynamic_slice_in_dim(queries, first_row, block_rows, 0).astype(jnp.float32)
        query_rows = query_rows.reshape(block_rows, KV_HEADS, group_ratio, HEAD_DIM)
        key_rows = lax.dynamic_slice_in_dim(padded_keys, first_row, block_rows + reach_back, 0).astype(jnp.float32)
        key_rows = key_rows.reshape(block_rows + reach_back, KV_HEADS, HEAD_DIM)
        value_rows = lax.dynamic_slice_in_dim(padded_values, first_row, block_rows + reach_back, 0).astype(jnp.float32)
        value_rows = value_rows.reshape(block_rows + reach_back, KV_HEADS, HEAD_DIM)
        query_docs = lax.dynamic_slice_in_dim(doc_ids.astype(jnp.int32), first_row, block_rows, 0)
        key_docs = lax.dynamic_slice_in_dim(padded_docs, first_row, block_rows + reach_back, 0)
        scores = jnp.einsum('bgrd,sgd->grbs', query_rows, key_rows) * score_scale
        offsets = jnp.arange(block_rows)[:, None] + reach_back - jnp.arange(block_rows + reach_back)[None, :]
        allowed = (offsets >= 0) & (offsets <= reach_back) & (query_docs[:, None] == key_docs[None, :])
        scores = jnp.where(allowed, scores, masked_score)
        row_max = jnp.maximum(scores.max(-1), sink_table)
        exp_scores = jnp.exp(scores - row_max[..., None])
        denominator = exp_scores.sum(-1) + jnp.exp(sink_table - row_max)
        probabilities = lax.optimization_barrier(exp_scores.astype(jnp.bfloat16)).astype(jnp.float32)
        weighted = jnp.einsum('grbs,sgd->bgrd', probabilities, value_rows)
        weighted = weighted / jnp.transpose(denominator, (2, 0, 1))[..., None]
        return weighted.astype(jnp.bfloat16).reshape(block_rows, HEADS * HEAD_DIM)
    attended = lax.map(attend_block, jnp.arange(SEQ // block_rows, dtype=jnp.int32)).reshape(SEQ, HEADS * HEAD_DIM)
    projected = jnp.dot(attended, out_weight, preferred_element_type=jnp.float32)
    stream = residual.astype(jnp.float32) + projected
    mean_value = stream.mean(-1, keepdims=True)
    centred = stream - mean_value
    variance = (centred * centred).mean(-1, keepdims=True)
    normed = (centred * lax.rsqrt(variance + layer_epsilon) * norm_gain.astype(jnp.float32)).astype(jnp.bfloat16)
    blocks_total = SEQ // TOK_DEV
    flat_routes = routes.astype(jnp.int32).reshape(blocks_total, TOP_K * TOK_DEV)
    one_hot = (flat_routes[..., None] == jnp.arange(EXPERTS, dtype=jnp.int32)).astype(jnp.int32)
    slot_ids = lax.optimization_barrier(jnp.sum((jnp.cumsum(one_hot, axis=1) - 1) * one_hot, axis=-1))
    block_base = jnp.arange(blocks_total, dtype=jnp.int32)[:, None] * CAP
    destination = (flat_routes * (blocks_total * CAP) + block_base + slot_ids).reshape(-1).astype(jnp.int32)
    token_index = (jnp.arange(SEQ * TOP_K, dtype=jnp.int32) // TOP_K).astype(jnp.int32)
    buffer_rows = jnp.zeros((EXPERTS * blocks_total * CAP, D), jnp.bfloat16).at[destination].set(normed[token_index])

    def run_expert(expert_index):
        rows_in = lax.dynamic_slice_in_dim(buffer_rows, (expert_index * blocks_total * CAP).astype(jnp.int32), blocks_total * CAP, 0)
        gate = jnp.dot(rows_in, gate_weight[expert_index], preferred_element_type=jnp.float32)
        upward = jnp.dot(rows_in, up_weight[expert_index], preferred_element_type=jnp.float32)
        hidden = (jax.nn.silu(gate) * upward).astype(jnp.bfloat16)
        grouped = hidden.reshape(blocks_total * CAP, N_TP, FF // N_TP).astype(jnp.float32)
        down_groups = down_weight[expert_index].reshape(N_TP, FF // N_TP, D).astype(jnp.float32)
        partials = jnp.einsum('rtf,tfd->trd', grouped, down_groups)
        rounded = lax.optimization_barrier(partials.astype(jnp.bfloat16)).astype(jnp.float32)
        return rounded.sum(0).astype(jnp.bfloat16)
    results = lax.map(run_expert, jnp.arange(EXPERTS, dtype=jnp.int32)).reshape(EXPERTS * blocks_total * CAP, D)
    picked = results[destination].astype(jnp.float32).reshape(SEQ, TOP_K, D)
    combined = lax.optimization_barrier(jnp.sum(picked * route_weights.astype(jnp.float32)[..., None], axis=1))
    return (stream + combined).astype(jnp.bfloat16)
```

```python
import math

import jax
import jax.numpy as jnp
from jax import lax
from jax.experimental import pallas as pl
from jax.experimental.layout import Layout, with_layout_constraint
from jax.experimental.pallas import tpu as pltpu
from jax.sharding import PartitionSpec as P


HEAD_DIM = 64
WINDOW = 128
CORES = 2
CHUNKS = 2

layer_epsilon = 1e-05
masked_score = -1e30


def passed_along(value, axis, steps):
    count = lax.axis_size(axis)
    first, last = (max(0, -steps), min(count, count - steps))
    return lax.ppermute(value, axis, [(source, source + steps) for source in range(first, last)])


def z_shift(value, steps):
    count = lax.axis_size("tp")
    return lax.ppermute(
        value, "tp", [(source, (source + CORES * steps) % count) for source in range(count)]
    )


def swap_cores(value):
    return lax.ppermute(value, "tp", [(source, source ^ 1) for source in range(lax.axis_size("tp"))])


def sp_exchange(value, flip):
    return lax.ppermute(value, "sp", [(source, source ^ flip) for source in range(lax.axis_size("sp"))])


def row_major(value):
    return with_layout_constraint(value, Layout(major_to_minor=tuple(range(value.ndim))))


def attend_kernel(sink_ref, query_ref, key_ref, value_ref, query_doc_ref, key_doc_ref, out_ref):
    heads_here = query_ref.shape[1] // HEAD_DIM
    group_ratio = query_ref.shape[1] // key_ref.shape[1]
    score_scale = 1.0 / math.sqrt(HEAD_DIM)
    offsets = (
        lax.broadcasted_iota(jnp.int32, (WINDOW, 2 * WINDOW), 0)
        + WINDOW
        - lax.broadcasted_iota(jnp.int32, (WINDOW, 2 * WINDOW), 1)
    )
    window_mask = (offsets >= 0) & (offsets < WINDOW)
    for block in range(query_ref.shape[0] // WINDOW):
        rows = pl.ds(block * WINDOW, WINDOW)
        reach = pl.ds(block * WINDOW, 2 * WINDOW)
        allowed = window_mask & (query_doc_ref[rows, :] == key_doc_ref[:, reach])
        pieces = []
        for head in range(heads_here):
            group = head // group_ratio
            columns = pl.ds(group * HEAD_DIM, HEAD_DIM)
            scores = lax.dot_general(
                query_ref[rows, pl.ds(head * HEAD_DIM, HEAD_DIM)],
                key_ref[reach, columns],
                (((1,), (1,)), ((), ())),
                preferred_element_type=jnp.float32,
            )
            scores = jnp.where(allowed, scores * score_scale, masked_score)
            sink = sink_ref[head]
            row_max = jnp.maximum(scores.max(-1, keepdims=True), sink)
            exp_scores = jnp.exp(scores - row_max)
            denominator = exp_scores.sum(-1, keepdims=True) + jnp.exp(sink - row_max)
            weighted = jnp.dot(
                exp_scores.astype(jnp.bfloat16),
                value_ref[reach, columns],
                preferred_element_type=jnp.float32,
            )
            pieces.append((weighted / denominator).astype(jnp.bfloat16))
        out_ref[rows, :] = jnp.concatenate(pieces, axis=1)


def attention(queries, keys, values, doc_ids, sink_logits):
    span_rows = queries.shape[0]
    kv_width = keys.shape[1]
    doc_float = (doc_ids + 1).astype(jnp.float32)
    doc_row = jnp.pad(doc_float[span_rows - WINDOW :], (0, 2 * kv_width - WINDOW))
    doc_rows = jnp.broadcast_to(doc_row.astype(jnp.bfloat16), (16, 2 * kv_width))
    tail = jnp.concatenate(
        [
            jnp.concatenate(
                [keys[span_rows - WINDOW :], values[span_rows - WINDOW :]], axis=1
            ),
            doc_rows,
        ],
        axis=0,
    )
    tail = passed_along(tail, "sp", 1)
    all_keys = jnp.concatenate([tail[:WINDOW, :kv_width], keys], axis=0)
    all_values = jnp.concatenate([tail[:WINDOW, kv_width:], values], axis=0)
    all_docs = jnp.concatenate([tail[WINDOW, :WINDOW].astype(jnp.float32), doc_float], axis=0)
    vmem = pl.BlockSpec(memory_space=pltpu.VMEM)
    return pl.pallas_call(
        attend_kernel,
        out_shape=jax.ShapeDtypeStruct(queries.shape, jnp.bfloat16),
        in_specs=[pl.BlockSpec(memory_space=pltpu.SMEM)] + [vmem] * 5,
        out_specs=vmem,
        name="attend",
    )(sink_logits, queries, all_keys, all_values, doc_float[:, None], all_docs[None, :])


def layer(
    queries,
    keys,
    values,
    doc_ids,
    sink_logits,
    out_weight,
    residual,
    norm_gain,
    routes,
    route_weights,
    gate_weight,
    up_weight,
    down_weight,
):
    tokens, width = residual.shape
    planes = lax.axis_size("tp") // CORES
    columns = lax.axis_size("sp")
    place = lax.axis_index("tp")
    plane, core = place // CORES, place % CORES
    column = lax.axis_index("sp")
    route_count = routes.shape[1]
    expert_count = columns * gate_weight.shape[0]
    capacity = 9 * route_count * tokens // (8 * expert_count)

    flat_routes = routes.reshape(-1)
    one_hot = (flat_routes[:, None] == jnp.arange(expert_count)[None, :]).astype(jnp.float32)
    order = jnp.arange(flat_routes.shape[0])
    before = (order[:, None] > order[None, :]).astype(jnp.float32)
    slot_ids = jnp.sum(jnp.dot(before, one_hot) * one_hot, axis=1).reshape(routes.shape)
    upper = route_weights.astype(jnp.bfloat16)
    lower = (route_weights - upper.astype(jnp.float32)).astype(jnp.bfloat16)
    table = jnp.concatenate(
        [routes.astype(jnp.bfloat16), slot_ids.astype(jnp.bfloat16), upper, lower], axis=1
    )
    table = jnp.pad(table, ((0, 0), (0, 128 - table.shape[1])))

    attended = attention(queries, keys, values, doc_ids, sink_logits)
    attended = attended.reshape(planes, CORES, tokens, -1)
    attended = jnp.concatenate([attended, attended[:, :1]], axis=1)
    attended = lax.dynamic_slice_in_dim(attended, core, CORES, 1)
    attended = jnp.concatenate([attended, attended[: planes - 1]], axis=0)
    attended = lax.dynamic_slice_in_dim(attended, plane, planes, 0)

    def project(which):
        return jnp.dot(
            attended[:, which].reshape(planes * tokens, -1),
            out_weight,
            preferred_element_type=jnp.float32,
        )

    theirs = row_major(swap_cores(row_major(project(1).astype(jnp.bfloat16))))
    summed = project(0) + theirs.astype(jnp.float32)
    outgoing = row_major(summed.astype(jnp.bfloat16))
    stream = residual.astype(jnp.float32) + summed[:tokens]
    sent = [
        row_major(z_shift(row_major(outgoing[step * tokens : (step + 1) * tokens]), step))
        for step in range(1, planes)
    ]
    for piece in sent:
        stream = stream + piece.astype(jnp.float32)
    mean_value = stream.mean(-1, keepdims=True)
    centred = stream - mean_value
    variance = (centred * centred).mean(-1, keepdims=True)
    normed = (centred * lax.rsqrt(variance + layer_epsilon) * norm_gain).astype(jnp.bfloat16)
    packet = jnp.concatenate([normed, table], axis=1)
    packets = [packet] + [z_shift(packet, step) for step in range(1, planes)]

    combined = stream
    chunks = CHUNKS if planes % CHUNKS == 0 else 1
    per_chunk = planes // chunks
    slots = per_chunk * capacity
    slot_range = jnp.arange(expert_count * slots)
    for chunk in range(chunks):
        held = jnp.concatenate(packets[chunk * per_chunk : (chunk + 1) * per_chunk], axis=0)
        entry = held[:, width:].astype(jnp.float32)
        expert = entry[:, :route_count].astype(jnp.int32)
        slot = entry[:, route_count : 2 * route_count].astype(jnp.int32)
        local_plane = jnp.arange(per_chunk * tokens)[:, None] // tokens
        hits = [
            (
                ((expert ^ column) * slots + local_plane * capacity + slot)[:, k : k + 1]
                == slot_range[None, :]
            )
            for k in range(route_count)
        ]
        selector = sum(hit.astype(jnp.float32) for hit in hits).astype(jnp.bfloat16)

        def mixer(first):
            return sum(
                jnp.where(hit, entry[:, first + k : first + k + 1], 0.0)
                for k, hit in enumerate(hits)
            ).astype(jnp.bfloat16)

        mixers = mixer(2 * route_count), mixer(3 * route_count)
        dispatch = lax.dot_general(
            selector,
            held[:, :width],
            (((0,), (0,)), ((), ())),
            preferred_element_type=jnp.float32,
        ).astype(jnp.bfloat16)
        arrived = [dispatch[:slots]] + [
            sp_exchange(dispatch[flip * slots : (flip + 1) * slots], flip)
            for flip in range(1, columns)
        ]
        arrived = jnp.concatenate(arrived, axis=0)
        rows = jnp.concatenate([arrived, swap_cores(arrived)], axis=0)
        half = arrived.shape[0]
        gate = jnp.dot(rows, gate_weight[0], preferred_element_type=jnp.float32)
        upward = jnp.dot(rows, up_weight[0], preferred_element_type=jnp.float32)
        hidden = (jax.nn.silu(gate) * upward).astype(jnp.bfloat16)
        outcome = jnp.dot(hidden, down_weight[0], preferred_element_type=jnp.float32).astype(
            jnp.bfloat16
        )
        other = swap_cores(outcome[half:])
        total = (outcome[:half].astype(jnp.float32) + other.astype(jnp.float32)).astype(
            jnp.bfloat16
        )
        back = [total[:slots]] + [
            sp_exchange(total[flip * slots : (flip + 1) * slots], flip)
            for flip in range(1, columns)
        ]
        back = jnp.concatenate(back, axis=0)
        share = jnp.dot(mixers[0], back, preferred_element_type=jnp.float32) + jnp.dot(
            mixers[1], back, preferred_element_type=jnp.float32
        )
        for local_index in range(per_chunk):
            step = chunk * per_chunk + local_index
            piece = share[local_index * tokens : (local_index + 1) * tokens]
            if step:
                piece = row_major(z_shift(row_major(piece.astype(jnp.bfloat16)), -step))
                piece = piece.astype(jnp.float32)
            combined = combined + piece
    return combined.astype(jnp.bfloat16)


def solution(mesh):
    placed = (
        P("sp", "tp"),
        P("sp", "tp"),
        P("sp", "tp"),
        P("sp"),
        P("tp"),
        P("tp", None),
        P(("sp", "tp"), None),
        P(),
        P(("sp", "tp"), None),
        P(("sp", "tp"), None),
        P("sp", None, "tp"),
        P("sp", None, "tp"),
        P("sp", "tp", None),
    )
    return jax.shard_map(
        layer, mesh=mesh, in_specs=placed, out_specs=P(("sp", "tp"), None), check_vma=False
    )
```
